128 devices in a mesh: sp: 64 (over z, y, x), tp: 2 (over core).
Axes of the slice: x: 4, y: 4, z: 4, core: 2. Of those that a mesh axis runs over, the one named last changes fastest.
Arguments:
- pool_input: bfloat16 [16384, 1024], P('sp', 'tp'), may hold values from -6 to 6
- residual: bfloat16 [16384, 2048], P(('sp', 'tp')), may hold values from -6 to 6
- pool_weight: bfloat16 [4, 256, 256], replicated, may hold values from -0.375 to 0.375
- pool_gain: float32 [1024], replicated, may hold values from 0.1 to 1.9
- out_weight: bfloat16 [1024, 2048], replicated, may hold values from -0.1875 to 0.1875
- norm_gain: float32 [2048], replicated, may hold values from 0.1 to 1.9
- routes: int32 [16384, 4], P(('sp', 'tp')), may hold values from 0 to 63, all different within a row; in each aligned block of 128 rows (0 to 127, 128 to 255, ...) at most 16 rows name the same one
- route_scores: float32 [16384, 4], P(('sp', 'tp')), may hold values from -1 to 1
- gate_weight: bfloat16 [64, 2048, 2048], P('sp', None, 'tp'), may hold values from -0.375 to 0.375
- up_weight: bfloat16 [64, 2048, 2048], P('sp', None, 'tp'), may hold values from -0.375 to 0.375
- down_weight: bfloat16 [64, 2048, 2048], P('sp', 'tp'), may hold values from -0.0234375 to 0.0234375
Outputs:
- layer_out: bfloat16 [16384, 2048], P(('sp', 'tp'))
The draws below stay inside these ranges and needn't reach their ends.
Inputs may be any that keep to these rules, and one draw needn't show every extreme that they name: `routes`: each row names 4 different experts; among the rows of one device no expert is named more than 16 times, a bound that some block reaches.
All inputs are finite; a program needn't handle non-finite values.
Results may differ from the reference program's by a relative error of at most 0.012.
Values may be sent and summed in bfloat16 or wider, within the bound.
No kernel may reach another device: no remote copies, remote signals or barrier semaphores. Data moves between devices by JAX's collectives and lax.ppermute only.
A program may use at most 128 MiB of HBM per device.

```python
import math
import jax
import jax.numpy as jnp
import numpy as np
from jax import lax

D = 2048
GROUPS = 4
GROUP_DIM = 256
FF = 2048
TOPK = 4
TOK_DEV = 256
PW = 1024
EXPERTS = 64
TOKENS = 16384
CAP = 16
N_TP = 2


def steps_of(own_key, shape, cuts, least, high):
    gain = 1.0
    for position, parts in cuts:
        draws = jax.random.uniform(jax.random.fold_in(jax.random.fold_in(own_key, 6), position), (parts,), jnp.float32, least / len(cuts), high / len(cuts))
        gain = gain * jnp.repeat(jnp.exp(draws), shape[position] // parts).reshape((-1,) + (1,) * (len(shape) - 1 - position))
    return gain


def shared_out(own_key, own, number, rows, amount, top, bound, lean):
    sequence = jax.random.permutation(own_key, amount)
    heavy_load, ordinary = shares(amount, rows * top, bound, lean, True), shares(amount, rows * top, bound, lean, False)
    places = jnp.arange(amount)

    def named(sizes, rotation):
        used = int((sizes > 0).sum())
        fixed = max(1, used // 4)
        passed = fixed + (places - fixed + rotation * (used - fixed)) % max(1, amount - fixed)
        return jnp.zeros((amount,), jnp.int32).at[sequence[jnp.where(places < fixed, places, passed)]].set(jnp.asarray(sizes, jnp.int32))

    sizes = jnp.where(number % 4 == 0, named(heavy_load, number // 4), named(ordinary, number - number // 4 - 1))
    mixed = jax.random.permutation(jax.random.fold_in(own, 3), amount)
    giver, receiver = mixed[0:amount // 2 * 2:2], mixed[1:amount // 2 * 2:2]
    room = jnp.minimum(sizes[giver] - 1, bound - sizes[receiver]) // 2
    room = jnp.where((giver == sequence[0]) | (receiver == sequence[0]) | (sizes[receiver] == 0), 0, jnp.maximum(room, 0))
    passed = jax.random.randint(jax.random.fold_in(own, 4), (amount // 2,), 0, 1 << 20) % (room + 1)
    sizes = sizes.at[giver].add(-passed).at[receiver].add(passed)
    members = jnp.searchsorted(jnp.cumsum(sizes), jnp.arange(rows * top), side="right").astype(jnp.int32)
    grid = members.reshape(top, rows).T
    grid = grid[jax.random.permutation(jax.random.fold_in(own, 1), rows)]
    rotation = jax.random.randint(jax.random.fold_in(own, 2), (rows, 1), 0, top)
    return jnp.take_along_axis(grid, (jnp.arange(top)[None, :] + rotation) % top, axis=1)


def shares(amount, total, bound, lean, full):
    loads = [(1 << 20) // math.isqrt(standing ** lean) + 1 for standing in range(1, amount + 1)]
    largest = bound if full else min(bound, max(-(-total // amount), total * loads[0] // sum(loads)))
    least = 1 if total - largest >= amount - 1 else 0
    given, rest = [largest] + [least] * (amount - 1), total - largest - least * (amount - 1)
    while rest > 0:
        candidates = [i for i in range(1, amount) if given[i] < largest] or [i for i in range(1, amount) if given[i] < bound]
        mass, left = sum([loads[i] for i in candidates]), rest
        for i in candidates:
            extra = min(bound - given[i], max(1, left * loads[i] // mass), rest)
            given[i] = given[i] + extra
            rest = rest - extra
    return np.array(given)


def bell_draw(rng, dims, spread, reach, cuts=(), dtype=jnp.bfloat16):
    factor_of = steps_of(rng, dims, cuts, -0.22, 0.18) if cuts else 1.0
    drawn = jax.random.normal(rng, dims, jnp.float32) * spread * factor_of
    return jnp.minimum(jnp.maximum(drawn, -reach), reach).astype(dtype)


def setup_inputs(seed: int = 0) -> dict:
    splits = jax.random.split(jax.random.key(seed), 12)
    pool_input = bell_draw(splits[0], (TOKENS, PW), 1.0, 6.0, ((0, 64), (1, 2)))
    residual = bell_draw(splits[1], (TOKENS, D), 1.0, 6.0, ((0, 128),))
    pool_weight = bell_draw(splits[2], (GROUPS, GROUP_DIM, GROUP_DIM), GROUP_DIM ** -0.5, 0.375)
    pool_gain = jnp.clip(1.0 + 0.18 * jax.random.normal(splits[3], (PW,), jnp.float32), 0.1, 1.9)
    out_weight = bell_draw(splits[4], (PW, D), PW ** -0.5, 0.1875)
    norm_gain = jnp.clip(1.0 + 0.18 * jax.random.normal(splits[5], (D,), jnp.float32), 0.1, 1.9)
    routes_keys = jax.random.split(jax.random.fold_in(splits[6], 1), TOKENS // (TOK_DEV // N_TP))
    routes_turns = jax.random.permutation(jax.random.fold_in(splits[6], 3), TOKENS // (TOK_DEV // N_TP))
    routes = jax.vmap(lambda own, number: shared_out(jax.random.fold_in(splits[6], 2), own, number, TOK_DEV // N_TP, EXPERTS, TOPK, CAP, 1))(routes_keys, routes_turns).reshape((TOKENS, TOPK))
    route_scores = bell_draw(splits[7], (TOKENS, TOPK), 0.4, 1.0, ((0, 128),), jnp.float32)
    gate_weight = bell_draw(splits[8], (EXPERTS, D, FF), (D // 9) ** -0.5, 0.375, ((0, 64), (2, 2)))
    up_weight = bell_draw(splits[9], (EXPERTS, D, FF), (D // 9) ** -0.5, 0.375, ((0, 64), (2, 2)))
    down_weight = bell_draw(splits[10], (EXPERTS, FF, D), (FF * 36) ** -0.5, 0.0234375, ((0, 64), (1, 2)))
    return {"pool_input": pool_input, "residual": residual, "pool_weight": pool_weight, "pool_gain": pool_gain, "out_weight": out_weight, "norm_gain": norm_gain, "routes": routes, "route_scores": route_scores, "gate_weight": gate_weight, "up_weight": up_weight, "down_weight": down_weight}


def expert_rows(rows, gate_matrix, up_matrix, down_matrix):
    gate_pre = jnp.dot(rows, gate_matrix, preferred_element_type=jnp.float32)
    up_pre = jnp.dot(rows, up_matrix, preferred_element_type=jnp.float32)
    clipped_gate = jnp.minimum(gate_pre, 7.0)
    clipped_up = jnp.clip(up_pre, -7.0, 7.0)
    activated = ((clipped_up + 1.0) * (clipped_gate * jax.nn.sigmoid(1.702 * clipped_gate))).astype(jnp.bfloat16)
    middle_unit = FF // 2
    first_half = jnp.dot(activated[:, :middle_unit], down_matrix[:middle_unit], preferred_element_type=jnp.float32).astype(jnp.bfloat16)
    second_half = jnp.dot(activated[:, middle_unit:], down_matrix[middle_unit:], preferred_element_type=jnp.float32).astype(jnp.bfloat16)
    first_half = lax.optimization_barrier(first_half)
    second_half = lax.optimization_barrier(second_half)
    return (first_half.astype(jnp.float32) + second_half.astype(jnp.float32)).astype(jnp.bfloat16)

def reference(pool_input, residual, pool_weight, pool_gain, out_weight, norm_gain, routes, route_scores, gate_weight, up_weight, down_weight):
    length = pool_input.shape[0]
    values = pool_input.astype(jnp.float32)
    padded = jnp.pad(values, ((16, 0), (0, 0)))
    positions = jnp.arange(length).astype(jnp.float32)
    pieces = []
    for group_index in range(GROUPS):
        window = 2 ** (group_index + 1)
        column = padded[:, group_index * GROUP_DIM:(group_index + 1) * GROUP_DIM]
        total = jnp.zeros((length, GROUP_DIM), jnp.float32)
        for offset in range(window):
            total = total + column[16 - offset:16 - offset + length]
        pieces.append(total / jnp.minimum(positions + 1.0, float(window))[:, None])
    pooled = (jnp.concatenate(pieces, axis=1) - values).astype(jnp.bfloat16)
    grouped = jnp.einsum('tgc,gce->tge', pooled.reshape(length, GROUPS, GROUP_DIM).astype(jnp.float32), pool_weight.astype(jnp.float32))
    mixer_out = (grouped.reshape(length, PW) * pool_gain[None, :]).astype(jnp.bfloat16)
    middle = (residual.astype(jnp.float32) + jnp.dot(mixer_out, out_weight, preferred_element_type=jnp.float32)).astype(jnp.bfloat16)
    middle_wide = middle.astype(jnp.float32)
    normed = (middle_wide * lax.rsqrt(lax.optimization_barrier(jnp.mean(middle_wide * middle_wide, axis=1, keepdims=True)) + 1e-05) * norm_gain[None, :]).astype(jnp.bfloat16)
    weights = jax.nn.softmax(route_scores.astype(jnp.float32), axis=-1)
    block_rows = 256
    count_routes = TOKENS * TOPK
    flat_expert = routes.reshape(-1).astype(jnp.int32)
    order = jnp.argsort(flat_expert, stable=True).astype(jnp.int32)
    sorted_expert = flat_expert[order]
    token_of = (order // TOPK).astype(jnp.int32)
    counts = lax.optimization_barrier(jnp.sum((flat_expert[:, None] == jnp.arange(EXPERTS).astype(jnp.int32)[None, :]).astype(jnp.int32), axis=0))
    starts = (jnp.cumsum(counts) - counts).astype(jnp.int32)
    padded_counts = ((counts + block_rows - 1) // block_rows * block_rows).astype(jnp.int32)
    ends = jnp.cumsum(padded_counts).astype(jnp.int32)
    begins = (ends - padded_counts).astype(jnp.int32)
    destination = (begins[sorted_expert] + jnp.arange(count_routes).astype(jnp.int32) - starts[sorted_expert]).astype(jnp.int32)
    blocks = -(-count_routes // block_rows) + EXPERTS
    slot_token = jnp.zeros((blocks * block_rows,), jnp.int32).at[destination].set(token_of)
    block_expert = jnp.minimum(jnp.searchsorted(ends, (jnp.arange(blocks) * block_rows).astype(jnp.int32), side='right'), EXPERTS - 1).astype(jnp.int32)

    def expert_block(operands):
        tokens_block, expert_id = operands
        return expert_rows(normed[tokens_block], gate_weight[expert_id], up_weight[expert_id], down_weight[expert_id])
    outputs = lax.map(expert_block, (slot_token.reshape(blocks, block_rows), block_expert)).reshape(blocks * block_rows, D)
    route_slot = jnp.zeros((count_routes,), jnp.int32).at[order].set(destination)
    route_rows = outputs[route_slot].astype(jnp.float32).reshape(TOKENS, TOPK, D)
    mixture = lax.optimization_barrier(jnp.sum(route_rows * weights[:, :, None], axis=1))
    return (middle_wide + mixture).astype(jnp.bfloat16)
```

```python
import jax
import jax.numpy as jnp
from jax import lax
from jax.sharding import PartitionSpec as P


def from_behind(block, axis, distance):
    devices = range(lax.axis_size(axis))
    route = [(i - distance, i) for i in devices if i - distance in devices]
    return lax.ppermute(block, axis, route)


def hidden_half(rows, gate_half, up_half):
    gate_pre = jnp.dot(rows, gate_half, preferred_element_type=jnp.float32)
    up_pre = jnp.dot(rows, up_half, preferred_element_type=jnp.float32)
    clipped_gate = jnp.minimum(gate_pre, 7.0)
    clipped_up = jnp.clip(up_pre, -7.0, 7.0)
    return ((clipped_up + 1.0) * (clipped_gate * jax.nn.sigmoid(1.702 * clipped_gate))).astype(
        jnp.bfloat16
    )


def shards(
    pool_input,
    residual,
    pool_weight,
    pool_gain,
    out_weight,
    norm_gain,
    routes,
    route_scores,
    gate_weight,
    up_weight,
    down_weight,
):
    swap = [(0, 1), (1, 0)]
    other_gate = lax.ppermute(gate_weight[0], "tp", swap)
    other_up = lax.ppermute(up_weight[0], "tp", swap)
    other_down = lax.ppermute(down_weight[0], "tp", swap)
    tokens_here, width_here = pool_input.shape
    cores = lax.axis_size("tp")
    groups_here = pool_weight.shape[0] // cores
    group_dim = pool_weight.shape[1]
    core_index = lax.axis_index("tp")
    first_group = core_index * groups_here
    previous = from_behind(pool_input[tokens_here - 16 :], "sp", 1)
    extended = jnp.concatenate([previous, pool_input], axis=0).astype(jnp.float32)
    channel_group = first_group + jnp.arange(width_here) // group_dim
    windows = jnp.left_shift(jnp.int32(2), channel_group).astype(jnp.float32)
    totals = jnp.zeros((tokens_here, width_here), jnp.float32)
    for offset in range(16):
        keeper = (windows > offset).astype(jnp.float32)
        totals = totals + extended[16 - offset : 16 - offset + tokens_here] * keeper[None, :]
    positions = (lax.axis_index("sp") * tokens_here + jnp.arange(tokens_here)).astype(jnp.float32)
    counts = jnp.minimum(positions[:, None] + 1.0, windows[None, :])
    pooled = (totals / counts - pool_input.astype(jnp.float32)).astype(jnp.bfloat16)
    local_weight = lax.dynamic_slice_in_dim(pool_weight, first_group, groups_here, 0)
    local_gain = lax.dynamic_slice_in_dim(pool_gain, first_group * group_dim, width_here, 0)
    grouped = jnp.einsum(
        "tgc,gce->tge",
        pooled.reshape(tokens_here, groups_here, group_dim),
        local_weight,
        preferred_element_type=jnp.float32,
    )
    mixer_out = (grouped.reshape(tokens_here, width_here) * local_gain[None, :]).astype(
        jnp.bfloat16
    )
    token_rows = lax.all_to_all(mixer_out, "tp", split_axis=0, concat_axis=1, tiled=True)
    projected = jnp.dot(token_rows, out_weight, preferred_element_type=jnp.float32)
    middle = (residual.astype(jnp.float32) + projected).astype(jnp.bfloat16)
    middle_wide = middle.astype(jnp.float32)
    normed = (
        middle_wide
        * lax.rsqrt(jnp.mean(middle_wide * middle_wide, axis=1, keepdims=True) + 1e-05)
        * norm_gain[None, :]
    ).astype(jnp.bfloat16)
    weights = jax.nn.softmax(route_scores, axis=-1)
    row_count, top_count = routes.shape
    model_width = normed.shape[1]
    experts_total = gate_weight.shape[0] * lax.axis_size("sp")
    capacity = row_count * top_count * cores // experts_total
    slots_total = experts_total * capacity
    flat_expert = routes.reshape(-1)
    onehot = (flat_expert[:, None] == jnp.arange(experts_total)[None, :]).astype(jnp.int32)
    ranks = jnp.sum((jnp.cumsum(onehot, axis=0) - 1) * onehot, axis=1)
    slot_ids = flat_expert * capacity + ranks
    picker = jnp.any(
        (jnp.arange(slots_total)[:, None] == slot_ids[None, :]).reshape(
            slots_total, row_count, top_count
        ),
        axis=2,
    ).astype(jnp.bfloat16)
    outgoing = (
        jnp.dot(picker, normed, preferred_element_type=jnp.float32)
        .astype(jnp.bfloat16)
        .reshape(experts_total, capacity, model_width)
    )
    received = lax.all_to_all(outgoing, "sp", split_axis=0, concat_axis=0, tiled=True)
    rows = received.reshape(-1, model_width)
    own = hidden_half(rows, gate_weight[0], up_weight[0])
    other = hidden_half(rows, other_gate, other_up)
    expert_rows = (
        jnp.dot(own, down_weight[0], preferred_element_type=jnp.float32)
        + jnp.dot(other, other_down, preferred_element_type=jnp.float32)
    ).astype(jnp.bfloat16)
    returned = lax.all_to_all(
        expert_rows.reshape(received.shape), "sp", split_axis=0, concat_axis=0, tiled=True
    ).reshape(slots_total, model_width)
    spread = jnp.sum(
        jnp.where(
            (jnp.arange(slots_total)[None, None, :] == slot_ids.reshape(row_count, top_count)[:, :, None]),
            weights[:, :, None],
            0.0,
        ),
        axis=1,
    )
    high = spread.astype(jnp.bfloat16)
    low = (spread - high.astype(jnp.float32)).astype(jnp.bfloat16)
    mixture = jnp.dot(high, returned, preferred_element_type=jnp.float32) + jnp.dot(
        low, returned, preferred_element_type=jnp.float32
    )
    return (middle_wide + mixture).astype(jnp.bfloat16)


def solution(mesh):
    return jax.shard_map(
        shards,
        mesh=mesh,
        in_specs=(
            P("sp", "tp"),
            P(("sp", "tp"), None),
            P(),
            P(),
            P(),
            P(),
            P(("sp", "tp"), None),
            P(("sp", "tp"), None),
            P("sp", None, "tp"),
            P("sp", None, "tp"),
            P("sp", "tp", None),
        ),
        out_specs=P(("sp", "tp"), None),
        check_vma=False,
    )
```

```python
import jax
import jax.numpy as jnp
from jax import lax
from jax.experimental import pallas as pl
from jax.experimental.pallas import tpu as pltpu
from jax.sharding import PartitionSpec as P

T = 256
R = 256
T2 = 256
HALO = 16
CAP = 16
PIECE = 256


def front_kernel(
    place_ref,
    halo_own,
    pool_input,
    halo_other,
    swapped,
    pool_weight,
    pool_gain,
    norm_gain,
    routes,
    out_weight_h,
    residual_h,
    outgoing_h,
    middle_ref,
    spot_ref,
    out_weight,
    residual,
    outgoing,
    s_weight,
    s_residual,
    s_out,
):
    rows = residual.shape[0]
    experts = spot_ref.shape[0]
    groups, group_dim, _ = pool_weight.shape
    weight_copy = pltpu.make_async_copy(out_weight_h, out_weight, s_weight)
    weight_copy.start()
    residual_copy = pltpu.make_async_copy(residual_h, residual, s_residual)
    residual_copy.start()
    core = place_ref[0]
    first = place_ref[1]
    lower = core == 0
    own = jnp.where(
        lower,
        jnp.concatenate([halo_own[...], pool_input[:rows, :]], axis=0).astype(jnp.float32),
        pool_input[rows - HALO :, :].astype(jnp.float32),
    )
    other = jnp.where(
        lower,
        jnp.concatenate([halo_other[...], swapped[:rows, :]], axis=0).astype(jnp.float32),
        swapped[...].astype(jnp.float32),
    )
    sides = (jnp.where(lower, own, other), jnp.where(lower, other, own))
    position = (first + 1 + lax.broadcasted_iota(jnp.int32, (rows, 1), 0)).astype(jnp.float32)
    mixed = []
    for group in range(groups):
        side = sides[group * 2 // groups]
        column = (group * group_dim) % side.shape[1]
        values = side[:, column : column + group_dim]
        total = values
        for step in range(group + 1):
            total = total + pltpu.roll(total, 1 << step, 0)
        window = float(2 << group)
        pooled = (total[HALO:] / jnp.minimum(position, window) - values[HALO:]).astype(jnp.bfloat16)
        grouped = jnp.dot(pooled, pool_weight[group], preferred_element_type=jnp.float32)
        span = slice(group * group_dim, (group + 1) * group_dim)
        mixed.append((grouped * pool_gain[:, span]).astype(jnp.bfloat16))
    expert_ids = lax.broadcasted_iota(jnp.int32, (experts, rows), 0)
    named = expert_ids == routes[0:1, :]
    for k in range(1, routes.shape[0]):
        named = jnp.logical_or(named, expert_ids == routes[k : k + 1, :])
    earlier = (
        lax.broadcasted_iota(jnp.int32, (rows, rows), 0)
        < lax.broadcasted_iota(jnp.int32, (rows, rows), 1)
    ).astype(jnp.float32).astype(jnp.bfloat16)
    ranks = jnp.dot(
        named.astype(jnp.float32).astype(jnp.bfloat16), earlier, preferred_element_type=jnp.float32
    )
    spot = jnp.where(named, ranks, -1.0)
    spot_ref[...] = spot
    picker = picked(spot).astype(jnp.bfloat16)
    weight_copy.wait()
    projected = jnp.dot(
        jnp.concatenate(mixed, axis=1), out_weight[...], preferred_element_type=jnp.float32
    )
    residual_copy.wait()
    middle = (residual[...].astype(jnp.float32) + projected).astype(jnp.bfloat16)
    middle_ref[...] = middle
    wide = middle.astype(jnp.float32)
    mean = jnp.mean(wide * wide, axis=1, keepdims=True)
    normed = (wide * lax.rsqrt(mean + 1e-05) * norm_gain[...]).astype(jnp.bfloat16)
    copies = []
    for piece in range(outgoing.shape[0] // PIECE):
        span = pl.ds(piece * PIECE, PIECE)
        outgoing[span, :] = jnp.dot(
            picker[piece * PIECE : (piece + 1) * PIECE], normed, preferred_element_type=jnp.float32
        ).astype(jnp.bfloat16)
        copy = pltpu.make_async_copy(outgoing.at[span], outgoing_h.at[span], s_out.at[piece])
        copy.start()
        copies.append(copy)
    for copy in copies:
        copy.wait()


def picked(spot):
    experts, rows = spot.shape
    slot = lax.broadcasted_iota(jnp.int32, (experts, CAP, rows), 1).astype(jnp.float32)
    chosen = jnp.broadcast_to(spot[:, None, :], (experts, CAP, rows)) == slot
    return jnp.where(chosen, 1.0, 0.0).reshape(experts * CAP, rows)


def front(place, halo_own, pool_input, halo_other, swapped, pool_weight, pool_gain, norm_gain, routes, out_weight, residual, experts):
    rows, width = residual.shape
    slots = experts * CAP
    vmem = pl.BlockSpec(memory_space=pltpu.VMEM)
    anywhere = pl.BlockSpec(memory_space=pl.ANY)
    return pl.pallas_call(
        front_kernel,
        out_shape=(
            jax.ShapeDtypeStruct((slots, width), jnp.bfloat16),
            jax.ShapeDtypeStruct((rows, width), jnp.bfloat16),
            jax.ShapeDtypeStruct((experts, rows), jnp.float32),
        ),
        in_specs=[pl.BlockSpec(memory_space=pltpu.SMEM)] + [vmem] * 8 + [anywhere] * 2,
        out_specs=(anywhere, vmem, vmem),
        scratch_shapes=[
            pltpu.VMEM(out_weight.shape, jnp.bfloat16),
            pltpu.VMEM((rows, width), jnp.bfloat16),
            pltpu.VMEM((slots, width), jnp.bfloat16),
            pltpu.SemaphoreType.DMA,
            pltpu.SemaphoreType.DMA,
            pltpu.SemaphoreType.DMA((slots // PIECE,)),
        ],
        cost_estimate=pl.CostEstimate(
            flops=4 * rows * width * slots, bytes_accessed=10 * slots * width // 2, transcendentals=0
        ),
        name="front",
    )(place, halo_own, pool_input, halo_other, swapped, pool_weight, pool_gain, norm_gain, routes, out_weight, residual)


def back_kernel(spot, routes, scores, middle, returned_h, out_ref, returned, sums, s_in):
    slots, width = returned.shape
    experts, rows = spot.shape
    pieces = slots // PIECE
    copies = []
    for piece in range(pieces):
        span = pl.ds(piece * PIECE, PIECE)
        copies.append(pltpu.make_async_copy(returned_h.at[span], returned.at[span], s_in.at[piece]))
        copies[-1].start()
    raised = jnp.exp(scores[...] - jnp.max(scores[...], axis=0, keepdims=True))
    weights = raised / jnp.sum(raised, axis=0, keepdims=True)
    expert_ids = lax.broadcasted_iota(jnp.int32, (experts, rows), 0)
    per_expert = jnp.zeros((experts, rows), jnp.float32)
    for k in range(routes.shape[0]):
        per_expert = per_expert + jnp.where(
            expert_ids == routes[k : k + 1, :], weights[k : k + 1, :], 0.0
        )
    spread = picked(spot[...]) * jnp.broadcast_to(
        per_expert[:, None, :], (experts, CAP, rows)
    ).reshape(slots, rows)
    spread = spread.T
    high = spread.astype(jnp.bfloat16)
    low = (spread - high.astype(jnp.float32)).astype(jnp.bfloat16)
    both = jnp.concatenate([high, low], axis=0)
    for piece in range(pieces):
        copies[piece].wait()
        part = jnp.dot(
            both[:, piece * PIECE : (piece + 1) * PIECE],
            returned[pl.ds(piece * PIECE, PIECE), :],
            preferred_element_type=jnp.float32,
        )
        part = part[:rows] + part[rows:]
        if piece == 0:
            sums[...] = part
        elif piece < pieces - 1:
            sums[...] += part
        else:
            out_ref[...] = (middle[...].astype(jnp.float32) + (sums[...] + part)).astype(jnp.bfloat16)


def back(spot, routes, scores, middle, returned):
    slots, width = returned.shape
    rows = middle.shape[0]
    vmem = pl.BlockSpec(memory_space=pltpu.VMEM)
    return pl.pallas_call(
        back_kernel,
        out_shape=jax.ShapeDtypeStruct((rows, width), jnp.bfloat16),
        in_specs=[vmem] * 4 + [pl.BlockSpec(memory_space=pl.ANY)],
        out_specs=vmem,
        scratch_shapes=[
            pltpu.VMEM((slots, width), jnp.bfloat16),
            pltpu.VMEM((rows, width), jnp.float32),
            pltpu.SemaphoreType.DMA((slots // PIECE,)),
        ],
        cost_estimate=pl.CostEstimate(
            flops=4 * rows * width * slots, bytes_accessed=2 * slots * width, transcendentals=0
        ),
        name="back",
    )(spot, routes, scores, middle, returned)


def activation(gate_pre, up_pre):
    clipped_gate = jnp.minimum(gate_pre, 7.0)
    clipped_up = jnp.clip(up_pre, -7.0, 7.0)
    return ((clipped_up + 1.0) * (clipped_gate * jax.nn.sigmoid(1.702 * clipped_gate))).astype(jnp.bfloat16)


def expert_kernel(rows_h, g0, u0, d0, g1, u1, d1, out_h, rows, act, wg, wu, wd, ob, sr, sg, su, sd, so):
    m, width = rows.shape
    half = g0.shape[1]
    n1 = half // T
    n2 = width // T2
    chunks = m // R
    def row_copy(c):
        return pltpu.make_async_copy(rows_h.at[pl.ds(c * R, R)], rows.at[pl.ds(c * R, R)], sr.at[c])
    def in_copies(gate, up, tile, slot):
        return (pltpu.make_async_copy(gate.at[:, pl.ds(tile * T, T)], wg.at[slot], sg.at[slot]),
                pltpu.make_async_copy(up.at[:, pl.ds(tile * T, T)], wu.at[slot], su.at[slot]))
    def down_copies(tile, slot):
        return (pltpu.make_async_copy(d0.at[:, pl.ds(tile * T2, T2)], wd.at[slot, pl.ds(0, half)], sd.at[slot, 0]),
                pltpu.make_async_copy(d1.at[:, pl.ds(tile * T2, T2)], wd.at[slot, pl.ds(half, half)], sd.at[slot, 1]))
    def fetch_in(step, slot):
        @pl.when(step < n1)
        def _():
            for c in in_copies(g0, u0, step, slot): c.start()
        @pl.when(jnp.logical_and(step >= n1, step < 2 * n1))
        def _():
            for c in in_copies(g1, u1, step - n1, slot): c.start()
    def fetch_down(step, slot):
        @pl.when(step < n2)
        def _():
            for c in down_copies(step, slot): c.start()
    first = in_copies(g0, u0, 0, 0)
    first[0].start(); row_copy(0).start(); first[1].start()
    for c in range(1, chunks): row_copy(c).start()
    fetch_in(1, 1)
    fetch_down(0, 0); fetch_down(1, 1)
    for c in range(chunks): row_copy(c).wait()
    @pl.loop(0, 2 * n1)
    def _(step):
        slot = step % 2
        for c in in_copies(g0, u0, 0, slot): c.wait()
        for c in range(chunks):
            part = rows[pl.ds(c * R, R), :]
            gate_pre = jnp.dot(part, wg[slot], preferred_element_type=jnp.float32)
            up_pre = jnp.dot(part, wu[slot], preferred_element_type=jnp.float32)
            act[step, pl.ds(c * R, R), :] = activation(gate_pre, up_pre)
        fetch_in(step + 2, slot)
    @pl.loop(0, n2)
    def _(step):
        slot = step % 2
        for c in down_copies(0, slot): c.wait()
        out_copy = pltpu.make_async_copy(ob.at[slot], out_h.at[:, pl.ds(step * T2, T2)], so.at[slot])
        @pl.when(step >= 2)
        def _(): out_copy.wait()
        for c in range(chunks):
            left = jnp.concatenate([act[s, pl.ds(c * R, R), :] for s in range(2 * n1)], axis=1)
            ob[slot, pl.ds(c * R, R), :] = jnp.dot(left, wd[slot], preferred_element_type=jnp.float32).astype(jnp.bfloat16)
        out_copy.start()
        fetch_down(step + 2, slot)
    for slot in range(2):
        pltpu.make_async_copy(ob.at[slot], out_h.at[:, pl.ds(0, T2)], so.at[slot]).wait()


def expert(rows, g0, u0, d0, g1, u1, d1):
    m, width = rows.shape
    half = g0.shape[1]
    anyspec = pl.BlockSpec(memory_space=pl.ANY)
    return pl.pallas_call(
        expert_kernel,
        out_shape=jax.ShapeDtypeStruct((m, width), jnp.bfloat16),
        in_specs=[anyspec] * 7,
        out_specs=anyspec,
        scratch_shapes=[
            pltpu.VMEM((m, width), jnp.bfloat16),
            pltpu.VMEM((2 * half // T, m, T), jnp.bfloat16),
            pltpu.VMEM((2, width, T), jnp.bfloat16),
            pltpu.VMEM((2, width, T), jnp.bfloat16),
            pltpu.VMEM((2, 2 * half, T2), jnp.bfloat16),
            pltpu.VMEM((2, m, T2), jnp.bfloat16),
            pltpu.SemaphoreType.DMA((m // R,)),
            pltpu.SemaphoreType.DMA((2,)),
            pltpu.SemaphoreType.DMA((2,)),
            pltpu.SemaphoreType.DMA((2, 2)),
            pltpu.SemaphoreType.DMA((2,)),
        ],
        cost_estimate=pl.CostEstimate(
            flops=12 * m * width * half,
            bytes_accessed=4 * m * width + 12 * width * half,
            transcendentals=2 * m * half,
        ),
        name="expert",
    )(rows, g0, u0, d0, g1, u1, d1)


def shards(
    pool_input,
    residual,
    pool_weight,
    pool_gain,
    out_weight,
    norm_gain,
    routes,
    route_scores,
    gate_weight,
    up_weight,
    down_weight,
):
    chips = lax.axis_size("sp")
    core = lax.axis_index("tp")
    rows, model_width = residual.shape
    experts = gate_weight.shape[0] * chips
    swap = [(0, 1), (1, 0)]
    both_axes = ("sp", "tp")
    tail_rows = pool_input[pool_input.shape[0] - HALO :]
    sent = lax.dynamic_slice_in_dim(pool_input, (1 - core) * (rows - HALO), rows + HALO, 0)
    halo_first = lax.ppermute(
        tail_rows, both_axes, [(2 * chip, 2 * chip + 2) for chip in range(chips - 1)]
    )
    halo_second = lax.ppermute(
        tail_rows, both_axes, [(2 * chip + 1, 2 * chip + 2) for chip in range(chips - 1)]
    )
    swapped = lax.ppermute(sent, "tp", swap)
    gate_own, up_own, down_own, halo_first, halo_second, swapped = lax.optimization_barrier(
        (gate_weight[0], up_weight[0], down_weight[0], halo_first, halo_second, swapped)
    )
    gate_other = lax.ppermute(gate_own, "tp", swap)
    up_other = lax.ppermute(up_own, "tp", swap)
    down_other = lax.ppermute(down_own, "tp", swap)
    place = jnp.stack([core, (lax.axis_index("sp") * 2 + core) * rows]).astype(jnp.int32)
    outgoing, middle, spot = front(
        place,
        halo_first,
        pool_input,
        halo_second,
        swapped,
        pool_weight,
        pool_gain[None, :],
        norm_gain[None, :],
        routes.T,
        out_weight,
        residual,
        experts,
    )
    received = lax.all_to_all(
        outgoing.reshape(experts, CAP, model_width), "sp", split_axis=0, concat_axis=0, tiled=True
    )
    expert_rows = expert(
        received.reshape(-1, model_width), gate_own, up_own, down_own, gate_other, up_other, down_other
    )
    returned = lax.all_to_all(
        expert_rows.reshape(received.shape), "sp", split_axis=0, concat_axis=0, tiled=True
    )
    return back(spot, routes.T, route_scores.T, middle, returned.reshape(-1, model_width))


def solution(mesh):
    return jax.shard_map(
        shards,
        mesh=mesh,
        in_specs=(
            P("sp", "tp"),
            P(("sp", "tp"), None),
            P(),
            P(),
            P(),
            P(),
            P(("sp", "tp"), None),
            P(("sp", "tp"), None),
            P("sp", None, "tp"),
            P("sp", None, "tp"),
            P("sp", "tp", None),
        ),
        out_specs=P(("sp", "tp"), None),
        check_vma=False,
    )
```
